32 devices in a mesh: kv: 8 (over z, y), tp: 4 (over x, core).
Axes of the slice: x: 2, y: 2, z: 4, core: 2. Of those that a mesh axis runs over, the one named last changes fastest.
Arguments:
- tokens: bfloat16 [8192, 1024], P('kv', 'tp'), may hold values from -6 to 6
- query_weight: bfloat16 [1024, 2048], P(None, 'tp'), may hold values from -0.1875 to 0.1875
- latent_weight: bfloat16 [1024, 128], replicated, may hold values from -0.1875 to 0.1875
- query_gain: float32 [128], replicated, may hold values from 0.5 to 1.5
- key_gain: float32 [128], replicated, may hold values from 0.5 to 1.5
- value_up: bfloat16 [16, 128, 64], P('tp'), may hold values from -0.5 to 0.5
- out_weight: bfloat16 [1024, 1024], P('tp'), may hold values from -0.25 to 0.25
- out_gain: float32 [1024], replicated, may hold values from 0.5 to 1.5
- chosen: int32 [64, 32], P('kv'), may hold values from -1 to 63, as said below
Outputs:
- mixed_out: bfloat16 [8192, 1024], P('kv', 'tp')
The draws below stay inside these ranges and needn't reach their ends.
Inputs may be any that keep to these rules, and one draw needn't show every extreme that they name: Row b lists the key blocks chosen for query block b: entry 0 is b itself, then distinct blocks before b, then -1 in every unused place. Block j is held by index j // 8 of kv. All query blocks of one index of kv together choose at most 2 distinct blocks held by any one other index, and some pair of indices reaches that bound; blocks held by the same index are chosen freely.
All inputs are finite; a program needn't handle non-finite values.
Results may differ from the reference program's by a relative error of at most 0.02.
Values may be sent and summed in bfloat16 or wider, within the bound.
A program may use at most 64 MiB of HBM per device.

```python
import jax
import jax.numpy as jnp
from jax import lax

D = 1024
HEADS = 16
LATENT = 128
VDIM = 64
BLOCK = 128
PICKS = 32
PER_OWNER = 2
TOKENS = 8192
BLOCKS_DEV = 8
BLOCKS = 64


def draw_chosen(key, part):
    per_dev = BLOCKS_DEV
    block_count = BLOCKS
    devices = block_count // per_dev
    level_key = jax.random.fold_in(key, 11)
    order_key = jax.random.fold_in(key, 12)
    pick_key = jax.random.fold_in(key, 13)
    classes = jax.random.randint(level_key, (devices,), 0, 4)
    levels = jnp.where(classes == 0, PER_OWNER, jnp.where(classes == 1, 1, 0)).astype(jnp.int32)
    levels = jnp.minimum(levels, PER_OWNER)
    levels = levels.at[0].set(PER_OWNER)
    block_ids = jnp.arange(block_count, dtype=jnp.int32)
    owner_ids = block_ids // per_dev
    local_ids = block_ids % per_dev
    raw_order = jax.random.randint(order_key, (devices, block_count), 0, 1 << 16)
    distinct = raw_order * per_dev + local_ids[None, :]
    grouped = distinct.reshape(devices, devices, per_dev)
    ranking = jnp.argsort(jnp.argsort(grouped, axis=2), axis=2).reshape(devices, block_count)
    requester = jnp.arange(devices, dtype=jnp.int32)
    allowed = (ranking < levels[owner_ids][None, :]) & (owner_ids[None, :] < requester[:, None])
    local_before = (owner_ids[None, :] == owner_ids[:, None]) & (block_ids[None, :] < block_ids[:, None])
    candidate = allowed[owner_ids] | local_before
    raw_pick = jax.random.randint(pick_key, (block_count, block_count), 0, 1 << 16)
    scores = jnp.where(candidate, raw_pick * block_count + block_ids[None, :], -1)
    best_scores, where_best = lax.top_k(scores, PICKS - 1)
    others = jnp.where(best_scores >= 0, where_best, -1).astype(jnp.int32)
    return jnp.concatenate([block_ids[:, None], others], axis=1).astype(jnp.int32)


def with_spikes(result, rng, source, target, shards_of, factor):
    def block_of(dim):
        return (jnp.arange(result.shape[dim]) // (result.shape[dim] // shards_of)).reshape((-1,) + (1,) * (result.ndim - 1 - dim))

    one_side = jax.random.permutation(rng, shards_of)[block_of(target)]
    far = (block_of(target) + shards_of // 2) % shards_of
    return jnp.where((block_of(source) == one_side) | (block_of(source) == far), factor * result, result)


def block_scale(stream_key, dims, cuts, smallest, high):
    gain = 1.0
    for position, shards_of in cuts:
        draws = jax.random.uniform(jax.random.fold_in(jax.random.fold_in(stream_key, 6), position), (shards_of,), jnp.float32, smallest / len(cuts), high / len(cuts))
        gain = gain * jnp.repeat(jnp.exp(draws), dims[position] // shards_of).reshape((-1,) + (1,) * (len(dims) - 1 - position))
    return gain


def bell_draw(own_key, dims, width, most, shards=(), kind=jnp.bfloat16):
    array = width * jax.random.normal(own_key, dims, jnp.float32)
    if shards:
        array = array * block_scale(own_key, dims, shards, -0.22, 0.18)
    return jnp.clip(array, -most, most).astype(kind)


def bell_draw_with(key, extent, width, limit, pieces, heavy, kind=jnp.bfloat16):
    drawn = width * jax.random.normal(key, extent, jnp.float32)
    if pieces:
        drawn = drawn * block_scale(key, extent, pieces, -0.22, 0.18)
    return jnp.clip(with_spikes(drawn, jax.random.fold_in(key, 3), *heavy), -limit, limit).astype(kind)


def setup_inputs(seed: int = 0) -> dict:
    splits = jax.random.split(jax.random.key(seed), 10)
    tokens = bell_draw(splits[0], (TOKENS, D), 1.0, 6.0, ((0, 8), (1, 4)))
    query_weight = bell_draw(splits[1], (D, HEADS * LATENT), D ** -0.5, 0.1875, ((1, 4),))
    latent_weight = bell_draw(splits[2], (D, LATENT), D ** -0.5, 0.1875)
    query_gain = jnp.clip(1.0 + 0.1 * jax.random.normal(splits[3], (LATENT,), jnp.float32), 0.5, 1.5)
    key_gain = jnp.clip(1.0 + 0.1 * jax.random.normal(splits[4], (LATENT,), jnp.float32), 0.5, 1.5)
    value_up = bell_draw(splits[5], (HEADS, LATENT, VDIM), LATENT ** -0.5, 0.5, ((0, 4),))
    out_weight = bell_draw_with(splits[6], (HEADS * VDIM, D), (HEADS * VDIM) ** -0.5, 0.25, ((0, 4),), (0, 1, 4, 2.0))
    out_gain = jnp.clip(1.0 + 0.1 * jax.random.normal(splits[7], (D,), jnp.float32), 0.5, 1.5)
    chosen = draw_chosen(jax.random.fold_in(splits[9], 71), 0)
    return {"tokens": tokens, "query_weight": query_weight, "latent_weight": latent_weight, "query_gain": query_gain, "key_gain": key_gain, "value_up": value_up, "out_weight": out_weight, "out_gain": out_gain, "chosen": chosen}


epsilon = 1e-06
masked_score = -1e+30

def rms_scale(values, gain_row):
    widened = values.astype(jnp.float32)
    mean_sq = lax.optimization_barrier(jnp.mean(widened * widened, axis=-1, keepdims=True))
    return (widened * lax.rsqrt(mean_sq + epsilon) * gain_row).astype(jnp.bfloat16)

def reference(tokens, query_weight, latent_weight, query_gain, key_gain, value_up, out_weight, out_gain, chosen):
    queries = jnp.dot(tokens, query_weight, preferred_element_type=jnp.float32).astype(jnp.bfloat16)
    queries = rms_scale(queries.reshape(TOKENS, HEADS, LATENT), query_gain)
    latent = jnp.dot(tokens, latent_weight, preferred_element_type=jnp.float32).astype(jnp.bfloat16)
    normed_keys = rms_scale(latent, key_gain)
    key_blocks = normed_keys.reshape(BLOCKS, BLOCK, LATENT)
    value_blocks = latent.reshape(BLOCKS, BLOCK, LATENT)
    query_blocks = queries.reshape(BLOCKS, BLOCK, HEADS, LATENT)
    offsets = jnp.arange(BLOCK, dtype=jnp.int32)

    def attend(packed):
        query_block, chosen_row, start_pos = packed
        clamped = jnp.maximum(chosen_row, 0).astype(jnp.int32)
        picked_keys = key_blocks[clamped].astype(jnp.float32)
        picked_values = value_blocks[clamped].astype(jnp.float32)
        scores = jnp.einsum('qhl,ckl->qhck', query_block.astype(jnp.float32), picked_keys) * LATENT ** (-0.5)
        key_pos = clamped[:, None] * BLOCK + offsets[None, :]
        query_pos = start_pos + offsets
        allowed = (chosen_row[:, None] >= 0)[None] & (key_pos[None] <= query_pos[:, None, None])
        allowed = allowed[:, None]
        scores = jnp.where(allowed, scores, masked_score)
        row_max = lax.optimization_barrier(jnp.max(scores, axis=(2, 3), keepdims=True))
        exp_scores = jnp.where(allowed, jnp.exp(scores - row_max), 0.0)
        weights = (exp_scores / lax.optimization_barrier(jnp.sum(exp_scores, axis=(2, 3), keepdims=True))).astype(jnp.bfloat16)
        attended = jnp.einsum('qhck,ckl->qhl', weights.astype(jnp.float32), picked_values)
        return attended.astype(jnp.bfloat16)
    block_starts = jnp.arange(BLOCKS, dtype=jnp.int32) * BLOCK
    attended = lax.map(attend, (query_blocks, chosen, block_starts))
    attended = attended.reshape(TOKENS, HEADS, LATENT)
    heads_out = jnp.einsum('thl,hlv->thv', attended.astype(jnp.float32), value_up.astype(jnp.float32))
    heads_out = heads_out.astype(jnp.bfloat16).reshape(TOKENS, HEADS * VDIM)
    projected = jnp.dot(heads_out, out_weight, preferred_element_type=jnp.float32)
    return rms_scale(projected, out_gain)
```

```python
import functools

import jax
import jax.numpy as jnp
from jax import lax
from jax.experimental import pallas as pl
from jax.experimental.pallas import tpu as pltpu
from jax.sharding import PartitionSpec as P

BLOCK = 128
PER_OWNER = 2


epsilon = 1e-06
masked_score = -1e30


def taken_in(shard, axis, dim, absorb, carry):
    whole = jax.tree.map(lambda part: lax.all_gather(part, axis, axis=dim, tiled=True), shard)
    return absorb(carry, whole, jnp.int32(0))


def own_rows(product, rows, axis):
    everything = product(jnp.int32(0), lax.axis_size(axis) * rows)
    own = lax.psum_scatter(everything.astype(jnp.bfloat16), axis, scatter_dimension=0, tiled=True)
    return own.astype(jnp.float32)


def rms_scale(values, gain_row):
    widened = values.astype(jnp.float32)
    mean_sq = jnp.mean(widened * widened, axis=-1, keepdims=True)
    return (widened * lax.rsqrt(mean_sq + epsilon) * gain_row).astype(jnp.bfloat16)


def norm_keys(pool_ref, gain_ref, kn_ref, vx_ref, rows):
    lat = pool_ref[rows, :]
    kn_ref[rows, :] = rms_scale(lat, gain_ref[...])
    vx_ref[rows, 0:lat.shape[1]] = lat
    vx_ref[rows, lat.shape[1] :] = jnp.ones_like(lat)


def attend_block(b, own_pairs, q_ref, kn_ref, vx_ref, bias_ref, p_ref, vu_ref):
    width = kn_ref.shape[1]
    heads = q_ref.shape[1] // width
    pairs = kn_ref.shape[0] // (2 * BLOCK)
    rows = pl.ds(pl.multiple_of(b * BLOCK, BLOCK), BLOCK)
    q = jnp.concatenate([q_ref[rows, h * width : (h + 1) * width] for h in range(heads)], axis=0)
    shape = (heads * BLOCK, 2 * BLOCK)
    row_pos = lax.broadcasted_iota(jnp.int32, shape, 0) % BLOCK + b * BLOCK
    col_pos = lax.broadcasted_iota(jnp.int32, shape, 1)
    for i in range(pairs):
        cols = slice(i * 2 * BLOCK, (i + 1) * 2 * BLOCK)
        s = lax.dot_general(
            q, kn_ref[cols, :], (((1,), (1,)), ((), ())), preferred_element_type=jnp.float32
        )
        s = s + bias_ref[b, :, cols]
        if i < own_pairs:
            s = jnp.where(col_pos + i * 2 * BLOCK <= row_pos, s, masked_score)
        p_ref[:, cols] = jnp.exp2(s).astype(jnp.bfloat16)
    acc = jnp.dot(p_ref[...], vx_ref[...], preferred_element_type=jnp.float32)
    att = (acc[:, :width] / acc[:, width:]).astype(jnp.bfloat16)
    out = []
    for h in range(0, heads, 2):
        two = jnp.concatenate(
            [att[h * BLOCK : (h + 1) * BLOCK], att[(h + 1) * BLOCK : (h + 2) * BLOCK]], axis=1
        )
        out.append(jnp.dot(two, vu_ref[h // 2], preferred_element_type=jnp.float32))
    return jnp.concatenate(out, axis=1).astype(jnp.bfloat16)


def attention_kernel(own_pairs, q_ref, pool_ref, bias_ref, gain_ref, vu_ref, o_ref, kn_ref, vx_ref, p_ref):
    @pl.loop(0, pool_ref.shape[0] // (2 * BLOCK))
    def _(i):
        norm_keys(pool_ref, gain_ref, kn_ref, vx_ref, pl.ds(pl.multiple_of(i * 2 * BLOCK, 2 * BLOCK), 2 * BLOCK))

    @pl.loop(0, q_ref.shape[0] // BLOCK)
    def _(b):
        o_ref[pl.ds(pl.multiple_of(b * BLOCK, BLOCK), BLOCK), :] = attend_block(
            b, own_pairs, q_ref, kn_ref, vx_ref, bias_ref, p_ref, vu_ref
        )


def paired_up(value_up):
    heads, width, vdim = value_up.shape
    pairs = value_up.reshape(heads // 2, 2, width, vdim)
    first = jnp.pad(pairs[:, 0], ((0, 0), (0, 0), (0, vdim)))
    second = jnp.pad(pairs[:, 1], ((0, 0), (0, 0), (vdim, 0)))
    return jnp.concatenate([first, second], axis=1)


def on_device(
    tokens,
    query_weight,
    latent_weight,
    query_gain,
    key_gain,
    value_up,
    out_weight,
    out_gain,
    chosen,
):
    tok_rows = tokens.shape[0]
    head_cols = query_weight.shape[1]
    lat_width = latent_weight.shape[1]
    local_heads = head_cols // lat_width
    block_size = BLOCK
    blocks_dev = tok_rows // block_size
    owners = lax.axis_size("kv")
    my_owner = lax.axis_index("kv")

    def project(totals, shard_piece, offset):
        query_rows = lax.dynamic_slice_in_dim(query_weight, offset, shard_piece.shape[1], 0)
        latent_rows = lax.dynamic_slice_in_dim(latent_weight, offset, shard_piece.shape[1], 0)
        return (
            totals[0] + jnp.dot(shard_piece, query_rows, preferred_element_type=jnp.float32),
            totals[1] + jnp.dot(shard_piece, latent_rows, preferred_element_type=jnp.float32),
        )

    query_zero = jnp.zeros((tok_rows, head_cols), jnp.float32)
    latent_zero = jnp.zeros((tok_rows, lat_width), jnp.float32)
    query_acc, latent_acc = taken_in(tokens, "tp", 1, project, (query_zero, latent_zero))
    scaled_gain = query_gain * (lat_width**-0.5 * 1.4426950408889634)
    queries = rms_scale(
        query_acc.astype(jnp.bfloat16).reshape(tok_rows, local_heads, lat_width), scaled_gain
    ).reshape(tok_rows, head_cols)
    latent = latent_acc.astype(jnp.bfloat16)
    latent_blocks = latent.reshape(blocks_dev, block_size, lat_width)
    clamped = jnp.maximum(chosen, 0)
    owner_of = clamped // blocks_dev
    index_in = clamped % blocks_dev
    flat_owner = owner_of.reshape(-1)
    flat_index = index_in.reshape(-1)
    remote = (chosen.reshape(-1) >= 0) & (flat_owner != my_owner)
    owner_ids = jnp.arange(owners, dtype=jnp.int32)
    local_ids = jnp.arange(blocks_dev, dtype=jnp.int32)
    matches = (
        remote[:, None, None]
        & (flat_owner[:, None, None] == owner_ids[None, :, None])
        & (flat_index[:, None, None] == local_ids[None, None, :])
    )
    needed = jnp.any(matches, axis=0)
    ranking = jnp.cumsum(needed.astype(jnp.int32), axis=1) - 1
    slot_ids = jnp.arange(PER_OWNER, dtype=jnp.int32)
    placed = needed[:, None, :] & (ranking[:, None, :] == slot_ids[None, :, None])
    wanted = jnp.where(
        jnp.any(placed, axis=2), jnp.sum(jnp.where(placed, local_ids[None, None, :], 0), axis=2), -1
    )
    requested = lax.all_to_all(wanted, "kv", split_axis=0, concat_axis=0, tiled=True)
    served = latent_blocks[jnp.maximum(requested, 0)]
    served = jnp.where((requested >= 0)[:, :, None, None], served, jnp.zeros_like(served))
    arrived = lax.all_to_all(served, "kv", split_axis=0, concat_axis=0, tiled=True)
    block_pool = jnp.concatenate(
        [latent_blocks, arrived.reshape(owners * PER_OWNER, block_size, lat_width)], axis=0
    )
    own_id = my_owner * blocks_dev + local_ids
    far_id = jnp.where(wanted >= 0, wanted + owner_ids[:, None] * blocks_dev, -2).reshape(-1)
    slot_block = jnp.concatenate([own_id, far_id])
    hit = jnp.any(chosen[:, :, None] == slot_block[None, None, :], axis=1)
    bias = jnp.repeat(jnp.where(hit, 0.0, masked_score), block_size, axis=1)[:, None, :]
    pool = block_pool.reshape(-1, lat_width)
    vdim = value_up.shape[2]
    heads_out = pl.pallas_call(
        functools.partial(attention_kernel, blocks_dev // 2),
        out_shape=jax.ShapeDtypeStruct((tok_rows, local_heads * vdim), jnp.bfloat16),
        in_specs=[pl.BlockSpec(memory_space=pltpu.VMEM)] * 5,
        out_specs=pl.BlockSpec(memory_space=pltpu.VMEM),
        scratch_shapes=[
            pltpu.VMEM(pool.shape, jnp.bfloat16),
            pltpu.VMEM((pool.shape[0], 2 * lat_width), jnp.bfloat16),
            pltpu.VMEM((local_heads * block_size, pool.shape[0]), jnp.bfloat16),
        ],
        compiler_params=pltpu.CompilerParams(vmem_limit_bytes=60 << 20),
    )(queries, pool, bias, key_gain[None, :], paired_up(value_up))
    model_width = out_weight.shape[1]
    tp_count = lax.axis_size("tp")
    feature_rows = model_width // tp_count
    gain_part = lax.dynamic_slice_in_dim(
        out_gain, lax.axis_index("tp") * feature_rows, feature_rows, 0
    )

    def columns(offset, count):
        weight_cols = lax.dynamic_slice_in_dim(out_weight, offset, count, 1)
        return lax.dot_general(
            weight_cols, heads_out, (((0,), (1,)), ((), ())), preferred_element_type=jnp.float32
        )

    summed = own_rows(columns, feature_rows, "tp").T
    squares = lax.psum(jnp.sum(summed * summed, axis=1), "tp")
    mixed_out = (summed * lax.rsqrt(squares / model_width + epsilon)[:, None] * gain_part).astype(
        jnp.bfloat16
    )
    return mixed_out


def solution(mesh):
    in_specs = (
        P("kv", "tp"),
        P(None, "tp"),
        P(),
        P(),
        P(),
        P("tp", None, None),
        P("tp", None),
        P(),
        P("kv", None),
    )
    out_specs = P("kv", "tp")
    return jax.shard_map(
        on_device, mesh=mesh, in_specs=in_specs, out_specs=out_specs, check_vma=False
    )
```

```python
import functools

import jax
import jax.numpy as jnp
from jax import lax
from jax.experimental import pallas as pl
from jax.experimental.pallas import tpu as pltpu
from jax.sharding import PartitionSpec as P

BLOCK = 128
PER_OWNER = 2
CHUNKS = 4
LAG = 2
MESH = pl.DeviceIdType.MESH

epsilon = 1e-06
masked_score = -1e30


def rms_scale(values, gain_row):
    widened = values.astype(jnp.float32)
    mean_sq = jnp.mean(widened * widened, axis=-1, keepdims=True)
    return (widened * lax.rsqrt(mean_sq + epsilon) * gain_row).astype(jnp.bfloat16)


def norm_keys(pool_ref, gain_ref, kn_ref, vx_ref, rows):
    lat = pool_ref[rows, :]
    kn_ref[rows, :] = rms_scale(lat, gain_ref[...])
    vx_ref[rows, 0:lat.shape[1]] = lat
    vx_ref[rows, lat.shape[1] :] = jnp.ones_like(lat)


def attend_block(b, own_pairs, q_ref, kn_ref, vx_ref, bias_ref, p_ref, vu_ref):
    width = kn_ref.shape[1]
    heads = q_ref.shape[1] // width
    pairs = kn_ref.shape[0] // (2 * BLOCK)
    rows = pl.ds(pl.multiple_of(b * BLOCK, BLOCK), BLOCK)
    q = jnp.concatenate([q_ref[rows, h * width : (h + 1) * width] for h in range(heads)], axis=0)
    shape = (heads * BLOCK, 2 * BLOCK)
    row_pos = lax.broadcasted_iota(jnp.int32, shape, 0) % BLOCK + b * BLOCK
    col_pos = lax.broadcasted_iota(jnp.int32, shape, 1)
    for i in range(pairs):
        cols = slice(i * 2 * BLOCK, (i + 1) * 2 * BLOCK)
        s = lax.dot_general(
            q, kn_ref[cols, :], (((1,), (1,)), ((), ())), preferred_element_type=jnp.float32
        )
        s = s + bias_ref[pl.ds(b, 1), cols]
        if i < own_pairs:
            s = jnp.where(col_pos + i * 2 * BLOCK <= row_pos, s, masked_score)
        p_ref[:, cols] = jnp.exp2(s).astype(jnp.bfloat16)
    acc = jnp.dot(p_ref[...], vx_ref[...], preferred_element_type=jnp.float32)
    att = (acc[:, :width] / acc[:, width:]).astype(jnp.bfloat16)
    out = []
    for h in range(0, heads, 2):
        two = jnp.concatenate(
            [att[h * BLOCK : (h + 1) * BLOCK], att[(h + 1) * BLOCK : (h + 2) * BLOCK]], axis=1
        )
        out.append(jnp.dot(two, vu_ref[h // 2], preferred_element_type=jnp.float32))
    return jnp.concatenate(out, axis=1).astype(jnp.bfloat16)


def paired_up(value_up):
    heads, width, vdim = value_up.shape
    pairs = value_up.reshape(heads // 2, 2, width, vdim)
    first = jnp.pad(pairs[:, 0], ((0, 0), (0, 0), (0, vdim)))
    second = jnp.pad(pairs[:, 1], ((0, 0), (0, 0), (vdim, 0)))
    return jnp.concatenate([first, second], axis=1)


def picked(table, first, count):
    found, rank = [], jnp.zeros((1, 1), jnp.float32)
    for j in range(count):
        rows = jnp.max(jnp.where(table == first + j, 1.0, 0.0), axis=1, keepdims=True)
        need = jnp.max(rows, axis=0, keepdims=True)
        found.append((rows, need, rank))
        rank = rank + need
    return found


def send(src, dst, sems, where):
    return pltpu.make_async_remote_copy(
        src_ref=src, dst_ref=dst, send_sem=sems[0], recv_sem=sems[1], device_id=where, device_id_type=MESH
    )


def kernel(
    kv_n, tp_n,
    tok_ref, wq_ref, wl_ref, qgain_ref, kgain_ref, vu_ref, w_ref, ogain_ref, chosen_ref,
    o_ref,
    tk_ref, q_ref, pool_ref, bias_ref, chs_ref, out_ref, kn_ref, vx_ref, p_ref,
    ho_ref, wc_ref, proj_ref, ss_ref, rs_ref,
    ch_s, ch_r, ts_s, ts_r, tx_s, tx_r, tr_s, tr_r, b_s, b_r, f_s, f_r,
    hs_s, hs_r, hx_s, hx_r, hr_s, hr_r, w_s, w_r, s_s, s_r,
):
    kv, tp = lax.axis_index("kv"), lax.axis_index("tp")
    core = lax.rem(tp, 2)
    sib = tp + 1 - 2 * core
    far = tp_n // 2 - 1
    toks, feat = tok_ref.shape
    width = wl_ref.shape[1]
    heads = wq_ref.shape[1] // width
    blocks = toks // BLOCK
    cols = o_ref.shape[1]
    crows = toks // CHUNKS

    def at_kv(other):
        return {"kv": other, "tp": tp}

    def at_tp(other):
        return {"kv": kv, "tp": other}

    def across(i, sign):
        return lax.rem(tp + sign * 2 * (i + 1) + tp_n, tp_n)

    barrier = pltpu.get_barrier_semaphore()
    for d in range(1, kv_n):
        pl.semaphore_signal(barrier, inc=1, device_id=at_kv(lax.rem(kv + d, kv_n)), device_id_type=MESH)
    for d in range(1, tp_n):
        pl.semaphore_signal(barrier, inc=1, device_id=at_tp(lax.rem(tp + d, tp_n)), device_id_type=MESH)
    pl.semaphore_wait(barrier, kv_n - 1 + tp_n - 1)

    def rows_of(c, n):
        return pl.ds(pl.multiple_of(c * n, n), n)

    def to_sib(src, buf, c, n, sems):
        return send(src.at[rows_of(c, n)], buf.at[tp, rows_of(c, n)], [s.at[c] for s in sems], at_tp(sib))

    def to_far(src, buf, c, n, i, sems):
        return send(
            src.at[rows_of(c, n)], buf.at[tp, rows_of(c, n)], [s.at[i, c] for s in sems], at_tp(across(i, 1))
        )

    def relay(buf, c, n, i, sems):
        part = buf.at[across(i, -1), rows_of(c, n)]
        return send(part, part, [s.at[i, c] for s in sems], at_tp(sib))

    def from_far(buf, c, n, i, sems):
        part = buf.at[across(i, -1), rows_of(c, n)]
        return send(part, part, [s.at[i, c] for s in sems], at_tp(sib))

    for c in range(CHUNKS):
        for i in range(far):
            to_far(tok_ref, tk_ref, c, crows, i, (tx_s, tx_r)).start()
        to_sib(tok_ref, tk_ref, c, crows, (ts_s, ts_r)).start()

    def ask(d):
        return send(chosen_ref, chs_ref.at[d - 1], (ch_s.at[d - 1], ch_r.at[d - 1]), at_kv(lax.rem(kv - d + kv_n, kv_n)))

    for d in range(1, kv_n):
        ask(d).start()

    tk_ref[tp] = tok_ref[...]
    table = chosen_ref[...]

    def put_bias(slot, hit):
        bias_ref[:, slot * BLOCK : (slot + 1) * BLOCK] = jnp.broadcast_to(
            (1.0 - hit) * masked_score, (blocks, BLOCK)
        )

    for j, (rows, _, _) in enumerate(picked(table, kv * blocks, blocks)):
        put_bias(j, rows)
    for d in range(1, kv_n):
        owner = kv - d
        first = jnp.where(owner >= 0, owner * blocks, -4 * blocks)
        found = picked(table, first, blocks)
        for k in range(PER_OWNER):
            hit = jnp.zeros((blocks, 1), jnp.float32)
            for rows, _, rank in found:
                hit = hit + jnp.where(rank == k, rows, 0.0)
            put_bias(blocks + (d - 1) * PER_OWNER + k, hit)

        @pl.when(owner < 0)
        def _(d=d):
            at = (blocks + (d - 1) * PER_OWNER) * BLOCK
            pool_ref[at : at + PER_OWNER * BLOCK, :] = jnp.zeros((PER_OWNER * BLOCK, width), jnp.bfloat16)

    gain = qgain_ref[...]

    def project(c):
        rows = slice(c * crows, (c + 1) * crows)
        x = jnp.concatenate([tk_ref[t, rows, :] for t in range(tp_n)], axis=1)
        lat = jnp.dot(x, wl_ref[...], preferred_element_type=jnp.float32)
        pool_ref[rows, :] = lat.astype(jnp.bfloat16)
        qs = jnp.dot(x, wq_ref[...], preferred_element_type=jnp.float32).astype(jnp.bfloat16)
        for h in range(heads):
            hc = slice(h * width, (h + 1) * width)
            q_ref[rows, hc] = rms_scale(qs[:, hc], gain)

    def arrive(c):
        to_sib(tok_ref, tk_ref, c, crows, (ts_s, ts_r)).wait()
        for i in range(far):
            relay(tk_ref, c, crows, i, (tr_s, tr_r)).wait()
            to_far(tok_ref, tk_ref, c, crows, i, (tx_s, tx_r)).wait_send()
        project(c)

    for c in range(CHUNKS):
        for i in range(far):
            from_far(tk_ref, c, crows, i, (tx_s, tx_r)).wait_recv()
            relay(tk_ref, c, crows, i, (tr_s, tr_r)).start()
        if c:
            arrive(c - 1)
    arrive(CHUNKS - 1)

    def weight(d):
        other = lax.rem(tp + d, tp_n)
        part = w_ref.at[:, pl.ds(pl.multiple_of(other * cols, cols), cols)]
        return send(part, wc_ref.at[tp], (w_s.at[d - 1], w_r.at[d - 1]), at_tp(other))

    def slot_rows(d, c):
        return pl.ds(pl.multiple_of((blocks + (d - 1) * PER_OWNER + c) * BLOCK, BLOCK), BLOCK)

    def give(d):
        return send(
            out_ref.at[d - 1], pool_ref.at[slot_rows(d, core)], (b_s.at[d - 1], b_r.at[d - 1]), at_kv(lax.rem(kv + d, kv_n))
        )

    def forward(d):
        part = pool_ref.at[slot_rows(d, core)]
        return send(part, part, (f_s.at[d - 1], f_r.at[d - 1]), at_tp(sib))

    mine = core.astype(jnp.float32)
    for d in range(1, kv_n):
        ask(d).wait()

        @pl.when(kv + d < kv_n)
        def _(d=d):
            total = jnp.zeros((BLOCK, width), jnp.float32)
            for j, (_, need, rank) in enumerate(picked(chs_ref[d - 1], kv * blocks, blocks)):
                share = jnp.where(rank == mine, need, 0.0)
                total = total + share * pool_ref[j * BLOCK : (j + 1) * BLOCK, :].astype(jnp.float32)
            out_ref[d - 1] = total.astype(jnp.bfloat16)
            give(d).start()

    for d in range(1, tp_n):
        weight(d).start()

    def norm(i):
        rows = pl.ds(pl.multiple_of(i * 2 * BLOCK, 2 * BLOCK), 2 * BLOCK)
        norm_keys(pool_ref, kgain_ref, kn_ref, vx_ref, rows)

    pl.loop(0, blocks // 2)(norm)
    wc_ref[tp] = w_ref[:, pl.ds(pl.multiple_of(tp * cols, cols), cols)]

    for d in range(1, kv_n):

        @pl.when(kv - d >= 0)
        def _(d=d):
            give(d).wait_recv()
            forward(d).start()

    for d in range(1, kv_n):

        @pl.when(kv - d >= 0)
        def _(d=d):
            forward(d).wait()

        norm(jnp.int32(blocks // 2 + d - 1))

    for d in range(1, kv_n):

        @pl.when(kv + d < kv_n)
        def _(d=d):
            give(d).wait_send()

    def hand_on(b):
        for i in range(far):
            from_far(ho_ref, b, BLOCK, i, (hx_s, hx_r)).wait_recv()
            relay(ho_ref, b, BLOCK, i, (hr_s, hr_r)).start()

    @pl.loop(0, blocks)
    def _(b):
        ho_ref[tp, rows_of(b, BLOCK), :] = attend_block(
            b, blocks // 2, q_ref, kn_ref, vx_ref, bias_ref, p_ref, vu_ref
        )
        for i in range(far):
            to_far(ho_ref.at[tp], ho_ref, b, BLOCK, i, (hx_s, hx_r)).start()
        to_sib(ho_ref.at[tp], ho_ref, b, BLOCK, (hs_s, hs_r)).start()

        @pl.when(b >= LAG)
        def _():
            hand_on(b - LAG)

    for d in range(1, tp_n):
        weight(d).wait()

    def finish(b):
        rows = rows_of(b, BLOCK)
        to_sib(ho_ref.at[tp], ho_ref, b, BLOCK, (hs_s, hs_r)).wait()
        for i in range(far):
            to_far(ho_ref.at[tp], ho_ref, b, BLOCK, i, (hx_s, hx_r)).wait_send()
            relay(ho_ref, b, BLOCK, i, (hr_s, hr_r)).wait()
        total = jnp.zeros((BLOCK, cols), jnp.float32)
        for t in range(tp_n):
            total = total + jnp.dot(ho_ref[t, rows, :], wc_ref[t], preferred_element_type=jnp.float32)
        proj_ref[rows, :] = total
        squares = jnp.sum(total * total, axis=1, keepdims=True)
        ss_ref[tp, pl.ds(b, 1), :] = jnp.broadcast_to(squares, (BLOCK, BLOCK)).T[0:1]

    for b in range(blocks - LAG, blocks):
        hand_on(b)
    pl.loop(0, blocks)(finish)

    def sums(d):
        return send(ss_ref.at[tp], ss_ref.at[tp], (s_s.at[d - 1], s_r.at[d - 1]), at_tp(lax.rem(tp + d, tp_n)))

    for d in range(1, tp_n):
        sums(d).start()
    for d in range(1, tp_n):
        sums(d).wait()
    total = ss_ref[0]
    for t in range(1, tp_n):
        total = total + ss_ref[t]
    rs_ref[...] = lax.rsqrt(total / (cols * tp_n) + epsilon)
    gains = ogain_ref[:, pl.ds(pl.multiple_of(tp * cols, cols), cols)]

    @pl.loop(0, blocks)
    def _(b):
        rows = rows_of(b, BLOCK)
        scale = jnp.broadcast_to(rs_ref[pl.ds(b, 1), :], (BLOCK, BLOCK)).T
        scale = jnp.concatenate([scale] * (cols // BLOCK), axis=1)
        o_ref[rows, :] = (proj_ref[rows, :] * scale * gains).astype(jnp.bfloat16)


def on_device(
    tokens,
    query_weight,
    latent_weight,
    query_gain,
    key_gain,
    value_up,
    out_weight,
    out_gain,
    chosen,
):
    toks, feat = tokens.shape
    width = latent_weight.shape[1]
    heads = query_weight.shape[1] // width
    blocks = toks // BLOCK
    kv_n, tp_n = lax.axis_size("kv"), lax.axis_size("tp")
    cols = out_weight.shape[1] // tp_n
    hv = out_weight.shape[0]
    far = tp_n // 2 - 1
    slots = blocks + (kv_n - 1) * PER_OWNER
    bf, f32 = jnp.bfloat16, jnp.float32
    wide = jnp.pad(chosen, ((0, 0), (0, BLOCK - chosen.shape[1])), constant_values=-1)
    scaled = (query_gain * (width**-0.5 * 1.4426950408889634))[None, :]
    dma = pltpu.SemaphoreType.DMA
    kvs, tps = [dma((kv_n - 1,))] * 2, [dma((tp_n - 1,))] * 2
    cs, cf = [dma((CHUNKS,))] * 2, [dma((far, CHUNKS))] * 2
    bs, bfar = [dma((blocks,))] * 2, [dma((far, blocks))] * 2
    return pl.pallas_call(
        functools.partial(kernel, kv_n, tp_n),
        out_shape=jax.ShapeDtypeStruct((toks, cols), bf),
        in_specs=[pl.BlockSpec(memory_space=pltpu.VMEM)] * 9,
        out_specs=pl.BlockSpec(memory_space=pltpu.VMEM),
        scratch_shapes=[
            pltpu.VMEM((tp_n, toks, feat), bf),
            pltpu.VMEM((toks, heads * width), bf),
            pltpu.VMEM((slots * BLOCK, width), bf),
            pltpu.VMEM((blocks, slots * BLOCK), f32),
            pltpu.VMEM((kv_n - 1, blocks, BLOCK), jnp.int32),
            pltpu.VMEM((kv_n - 1, BLOCK, width), bf),
            pltpu.VMEM((slots * BLOCK, width), bf),
            pltpu.VMEM((slots * BLOCK, 2 * width), bf),
            pltpu.VMEM((heads * BLOCK, slots * BLOCK), bf),
            pltpu.VMEM((tp_n, toks, hv), bf),
            pltpu.VMEM((tp_n, hv, cols), bf),
            pltpu.VMEM((toks, cols), f32),
            pltpu.VMEM((tp_n, blocks, BLOCK), f32),
            pltpu.VMEM((blocks, BLOCK), f32),
            *kvs, *cs, *cf, *cf, *kvs, *kvs, *bs, *bfar, *bfar, *tps, *tps,
        ],
        compiler_params=pltpu.CompilerParams(
            collective_id=0, has_side_effects=True, vmem_limit_bytes=60 << 20
        ),
    )(
        tokens, query_weight, latent_weight, scaled, key_gain[None, :], paired_up(value_up),
        out_weight, out_gain[None, :], wide,
    )


def solution(mesh):
    in_specs = (
        P("kv", "tp"),
        P(None, "tp"),
        P(),
        P(),
        P(),
        P("tp", None, None),
        P("tp", None),
        P(),
        P("kv", None),
    )
    out_specs = P("kv", "tp")
    return jax.shard_map(
        on_device, mesh=mesh, in_specs=in_specs, out_specs=out_specs, check_vma=False
    )
```
